32 devices in a mesh: rep: 2 (over x), fs: 8 (over z, y), tp: 2 (over core).
Axes of the slice: x: 2, y: 2, z: 4, core: 2. Of those that a mesh axis runs over, the one named last changes fastest.
Arguments:
- inputs: bfloat16 [8192, 2048], P(('rep', 'fs')), may hold values from -6 to 6
- gain: float32 [2048], replicated, may hold values from 0.1 to 1.9
- gate_weight: bfloat16 [2048, 3072], P('fs', 'tp'), may hold values from -0.125 to 0.125
- up_weight: bfloat16 [2048, 3072], P('fs', 'tp'), may hold values from -0.125 to 0.125
- down_weight: bfloat16 [2048, 3072], P('fs', 'tp'), may hold values from -0.109375 to 0.109375
- cotangent: bfloat16 [8192, 2048], P(('rep', 'fs')), may hold values from -6 to 6
Outputs:
- input_gradient: bfloat16 [8192, 2048], P(('rep', 'fs'))
- gain_gradient: float32 [2048], replicated
- d_down: float32 [2048, 3072], P('fs', 'tp')
The draws below stay inside these ranges and needn't reach their ends.
All inputs are finite; a program needn't handle non-finite values.
Results may differ from the reference program's by a relative error of at most 0.014.
Values may be sent and summed in bfloat16 or wider, within the bound.
A program may use at most 128 MiB of HBM per device.

```python
import jax
import jax.numpy as jnp
from jax import lax

D = 2048
FF = 3072
TOKENS = 8192
N_TP = 2


def with_spikes(result, stream_key, source, target, blocks, factor):
    owner, partner = [(jnp.arange(result.shape[dim]) // (result.shape[dim] // blocks)).reshape([-1 if axis == dim else 1 for axis in range(result.ndim)]) for dim in (source, target)]
    chosen = jax.random.permutation(stream_key, blocks)[partner]
    strong = (owner == chosen) | (owner == (partner + blocks // 2) % blocks)
    return jnp.where(strong, factor * result, result)


def shard_levels(rng, dims, split, least, high):
    def one(dim, parts):
        steps = jax.random.uniform(jax.random.fold_in(jax.random.fold_in(rng, 6), dim), (parts,), jnp.float32, least / len(split), high / len(split))
        return jnp.repeat(jnp.exp(steps), dims[dim] // parts).reshape((-1,) + (1,) * (len(dims) - dim - 1))

    factor_of = one(*split[0])
    for cut in split[1:]:
        factor_of = factor_of * one(*cut)
    return factor_of


def gaussian(rng, shape, width, bound, split=(), dtype=jnp.bfloat16):
    drawn = width * jax.random.normal(rng, shape, jnp.float32)
    if split:
        drawn = drawn * shard_levels(rng, shape, split, -0.22, 0.18)
    return jnp.clip(drawn, -bound, bound).astype(dtype)


def bell_draw_with(stream_key, extent, scale, reach, cuts, heavy, held_as=jnp.bfloat16):
    array = scale * jax.random.normal(stream_key, extent, jnp.float32)
    if cuts:
        array = array * shard_levels(stream_key, extent, cuts, -0.22, 0.18)
    return jnp.clip(with_spikes(array, jax.random.fold_in(stream_key, 3), *heavy), -reach, reach).astype(held_as)


def setup_inputs(seed: int = 0) -> dict:
    key_of = jax.random.split(jax.random.key(seed), 7)
    inputs = gaussian(key_of[0], (TOKENS, D), 1.0, 6.0, ((0, 16),))
    gain = jnp.clip(1.0 + 0.18 * jax.random.normal(key_of[1], (D,), jnp.float32), 0.1, 1.9)
    gate_weight = gaussian(key_of[2], (D, FF), D ** -0.5, 0.125, ((0, 8), (1, 2)))
    up_weight = gaussian(key_of[3], (D, FF), D ** -0.5, 0.125, ((0, 8), (1, 2)))
    down_weight = gaussian(key_of[4], (D, FF), FF ** -0.5, 0.109375, ((0, 8), (1, 2)))
    cotangent = bell_draw_with(key_of[5], (TOKENS, D), 1.0, 6.0, ((0, 16),), (0, 1, 16, 2.0))
    return {"inputs": inputs, "gain": gain, "gate_weight": gate_weight, "up_weight": up_weight, "down_weight": down_weight, "cotangent": cotangent}


EPS = 1e-06

def reference(inputs, gain, gate_weight, up_weight, down_weight, cotangent):
    single_precision = inputs.astype(jnp.float32)
    reciprocal_root_mean = lax.rsqrt(lax.optimization_barrier(jnp.mean(single_precision * single_precision, axis=-1, keepdims=True)) + EPS)
    unit_input = single_precision * reciprocal_root_mean
    normalized_input = (unit_input * gain).astype(jnp.bfloat16)
    gate = jnp.dot(normalized_input, gate_weight, preferred_element_type=jnp.float32)
    up_proj = jnp.dot(normalized_input, up_weight, preferred_element_type=jnp.float32)
    gate_sig = jax.nn.sigmoid(gate)
    active = gate * gate_sig
    hidden = (active * up_proj).astype(jnp.bfloat16)
    d_hidden = 0.5 * lax.dot_general(cotangent, down_weight, (((1,), (0,)), ((), ())), preferred_element_type=jnp.float32)
    d_down = 0.5 * lax.dot_general(cotangent, hidden, (((0,), (0,)), ((), ())), preferred_element_type=jnp.float32)
    d_gate = (d_hidden * up_proj * gate_sig * (1.0 + gate * (1.0 - gate_sig))).astype(jnp.bfloat16)
    d_up = (d_hidden * active).astype(jnp.bfloat16)
    unit_width = FF // N_TP
    normalized_gradient = jnp.zeros(single_precision.shape, jnp.float32)
    for column_block in range(N_TP):
        first = column_block * unit_width
        partial_value = lax.dot_general(d_gate[:, first:first + unit_width], gate_weight[:, first:first + unit_width], (((1,), (1,)), ((), ())), preferred_element_type=jnp.float32)
        partial_value = partial_value + lax.dot_general(d_up[:, first:first + unit_width], up_weight[:, first:first + unit_width], (((1,), (1,)), ((), ())), preferred_element_type=jnp.float32)
        rounded = lax.optimization_barrier(partial_value.astype(jnp.bfloat16))
        normalized_gradient = normalized_gradient + rounded.astype(jnp.float32)
    summed_rounded = lax.optimization_barrier(normalized_gradient.astype(jnp.bfloat16))
    normalized_gradient = summed_rounded.astype(jnp.float32)
    gain_gradient = lax.optimization_barrier(jnp.sum(normalized_gradient * unit_input, axis=0))
    gain_scaled = gain * normalized_gradient
    mean_correction = lax.optimization_barrier(jnp.mean(gain_scaled * unit_input, axis=-1, keepdims=True))
    input_gradient = (cotangent.astype(jnp.float32) + reciprocal_root_mean * (gain_scaled - unit_input * mean_correction)).astype(jnp.bfloat16)
    return (input_gradient, gain_gradient, d_down)
```

```python
import jax
import jax.numpy as jnp
from jax import lax
from jax.sharding import PartitionSpec as P

EPS = 1e-06


def shift(value, axis, step):
    size = lax.axis_size(axis)
    return lax.ppermute(value, axis, [(i, (i + step) % size) for i in range(size)])


def local(inputs, gain, gate_weight, up_weight, down_weight, cotangent):
    n_rep, n_tp = lax.axis_size("rep"), lax.axis_size("tp")
    rep, tp = lax.axis_index("rep"), lax.axis_index("tp")
    rows, width = inputs.shape
    block = rows // n_tp
    units = gate_weight.shape[1] // n_rep

    def own_units(weight):
        return lax.dynamic_slice_in_dim(weight, rep * units, units, axis=1)

    def own_block(value, step):
        return lax.dynamic_slice_in_dim(value, (tp + step) % n_tp * block, block, axis=0)

    def gathered_tokens(value):
        parts = [own_block(value, s) for s in range(n_tp)]
        for j in range(1, n_rep):
            first = shift(own_block(value, 0), "rep", -j)
            parts += [first] + [shift(first, "tp", -s) for s in range(1, n_tp)]
        return jnp.concatenate(parts, axis=0)

    gate_full = lax.all_gather(own_units(gate_weight), "fs", axis=0, tiled=True)
    up_full = lax.all_gather(own_units(up_weight), "fs", axis=0, tiled=True)
    down_full = lax.all_gather(own_units(down_weight), "fs", axis=0, tiled=True)

    tokens = gathered_tokens(inputs)
    cots = gathered_tokens(cotangent)

    def normed(value):
        single = value.astype(jnp.float32)
        inv = lax.rsqrt(jnp.mean(single * single, axis=-1, keepdims=True) + EPS)
        return single * inv, inv

    normalized_input = (normed(tokens)[0] * gain).astype(jnp.bfloat16)
    contract_cols = (((1,), (1,)), ((), ()))
    contract_rows = (((0,), (0,)), ((), ()))
    gate = jnp.dot(normalized_input, gate_full, preferred_element_type=jnp.float32)
    up_proj = jnp.dot(normalized_input, up_full, preferred_element_type=jnp.float32)
    gate_sig = jax.nn.sigmoid(gate)
    active = gate * gate_sig
    hidden = (active * up_proj).astype(jnp.bfloat16)
    summed = lax.psum_scatter(
        (0.5 * lax.dot_general(cots, hidden, contract_rows, preferred_element_type=jnp.float32)).astype(jnp.bfloat16),
        "fs",
        scatter_dimension=0,
        tiled=True,
    )
    d_hidden = 0.5 * jnp.dot(cots, down_full, preferred_element_type=jnp.float32)
    d_gate = (d_hidden * up_proj * gate_sig * (1.0 + gate * (1.0 - gate_sig))).astype(jnp.bfloat16)
    d_up = (d_hidden * active).astype(jnp.bfloat16)
    partial_value = (
        lax.dot_general(d_gate, gate_full, contract_cols, preferred_element_type=jnp.float32)
        + lax.dot_general(d_up, up_full, contract_cols, preferred_element_type=jnp.float32)
    ).astype(jnp.bfloat16).reshape(n_rep, n_tp, block, width)
    over_tp = partial_value[:, 0].astype(jnp.float32)
    for s in range(1, n_tp):
        over_tp = over_tp + shift(partial_value[:, s], "tp", s).astype(jnp.float32)
    over_tp = over_tp.astype(jnp.bfloat16)
    total = over_tp[0].astype(jnp.float32)
    for j in range(1, n_rep):
        total = total + shift(over_tp[j], "rep", j).astype(jnp.float32)
    normalized_gradient = total.astype(jnp.bfloat16).astype(jnp.float32)
    unit_input, inv = normed(own_block(inputs, 0))
    gain_gradient = lax.psum(
        jnp.sum(normalized_gradient * unit_input, axis=0), ("rep", "fs", "tp")
    )
    gain_scaled = gain * normalized_gradient
    mean_correction = jnp.mean(gain_scaled * unit_input, axis=-1, keepdims=True)
    block_gradient = (
        own_block(cotangent, 0).astype(jnp.float32)
        + inv * (gain_scaled - unit_input * mean_correction)
    ).astype(jnp.bfloat16)
    input_gradient = jnp.zeros((rows, width), jnp.bfloat16)
    for s in range(n_tp):
        piece = block_gradient if s == 0 else shift(block_gradient, "tp", -s)
        input_gradient = lax.dynamic_update_slice_in_dim(
            input_gradient, piece, (tp + s) % n_tp * block, axis=0
        )
    d_down = jnp.zeros((summed.shape[0], units * n_rep), jnp.float32)
    for j in range(n_rep):
        piece = summed if j == 0 else shift(summed, "rep", -j)
        d_down = lax.dynamic_update_slice_in_dim(
            d_down, piece.astype(jnp.float32), (rep + j) % n_rep * units, axis=1
        )
    return (input_gradient, gain_gradient, d_down)


def solution(mesh):
    placed = (
        P(("rep", "fs"), None),
        P(),
        P("fs", "tp"),
        P("fs", "tp"),
        P("fs", "tp"),
        P(("rep", "fs"), None),
    )
    return jax.shard_map(
        local,
        mesh=mesh,
        in_specs=placed,
        out_specs=(P(("rep", "fs"), None), P(), P("fs", "tp")),
        check_vma=False,
    )
```
